128 devices in a mesh: ep: 128 (over z, y, x, core).
Axes of the slice: x: 4, y: 4, z: 4, core: 2. Of those that a mesh axis runs over, the one named last changes fastest.
Arguments:
- tokens: bfloat16 [16384, 2048], P('ep'), may hold values from -6 to 6
- norm_gain: float32 [2048], replicated, may hold values from 0.1 to 1.9
- expert_ids: int32 [16384, 4], P('ep'), may hold values from 0 to 255, as said below
- gate_weights: float32 [16384, 4], P('ep'), may hold values from 0.1 to 0.6
- expert_gate: bfloat16 [256, 2048, 512], P('ep'), may hold values from -0.125 to 0.125
- expert_up: bfloat16 [256, 2048, 512], P('ep'), may hold values from -0.125 to 0.125
- expert_down: bfloat16 [256, 512, 2048], P('ep'), may hold values from -0.25 to 0.25
- shared_gate: bfloat16 [2048, 512], P('ep'), may hold values from -0.125 to 0.125
- shared_up: bfloat16 [2048, 512], P('ep'), may hold values from -0.125 to 0.125
- shared_down: bfloat16 [512, 2048], P(None, 'ep'), may hold values from -0.25 to 0.25
Outputs:
- mixed: bfloat16 [16384, 2048], P('ep')
The draws below stay inside these ranges and needn't reach their ends.
Inputs may be any that keep to these rules, and one draw needn't show every extreme that they name: `expert_ids`: expert e belongs to device e // 2; each row names 4 experts of 4 different devices; among the rows of one device at most 6 name experts of any one device, hence at most 6 any one expert; in every aligned block of 128 rows exactly 6 rows name one and the same expert.
All inputs are finite; a program needn't handle non-finite values.
Results may differ from the reference program's by a relative error of at most 0.0067.
Values may be sent and summed in bfloat16 or wider, within the bound.
A program may use at most 128 MiB of HBM per device.

```python
import jax
import jax.numpy as jnp
from jax import lax

D = 2048
DE = 512
DS = 512
TOP_K = 4
EXP_DEV = 2
TOK_DEV = 128
EXPERTS = 256
TOKENS = 16384


def route_block(block_key):
    holders = EXPERTS // EXP_DEV
    total = TOK_DEV * TOP_K
    mean_rows = total // holders
    extra = mean_rows // 2
    key_order, key_moved, key_bits, key_rows = jax.random.split(block_key, 4)
    order = jax.random.permutation(key_order, holders).astype(jnp.int32)
    moved = jax.random.randint(key_moved, (holders // 2,), 0, extra + 1).astype(jnp.int32)
    moved = moved.at[0].set(extra)
    counts = jnp.full((holders,), mean_rows, jnp.int32)
    counts = counts.at[order[0::2]].add(moved).at[order[1::2]].add(-moved)
    ends = jnp.cumsum(counts).astype(jnp.int32)
    slots = jnp.arange(total, dtype=jnp.int32)
    slot_dev = jnp.sum((ends[None, :] <= slots[:, None]).astype(jnp.int32), axis=1).astype(jnp.int32)
    bits = jax.random.randint(key_bits, (total,), 0, EXP_DEV).astype(jnp.int32)
    bits = jnp.where(slot_dev == order[0], 0, bits).astype(jnp.int32)
    expert = (slot_dev * EXP_DEV + bits).astype(jnp.int32)
    row_perm = jax.random.permutation(key_rows, TOK_DEV).astype(jnp.int32)
    row_of = row_perm[slots % TOK_DEV]
    column = (slots // TOK_DEV).astype(jnp.int32)
    table = jnp.zeros((TOK_DEV, TOP_K), jnp.int32).at[row_of, column].set(expert)
    return table


def draw_expert_ids(key, part):
    base = jax.random.fold_in(key, 7117)
    keys = jax.random.split(base, TOKENS // TOK_DEV)
    tables = jax.vmap(route_block)(keys)
    return tables.reshape(TOKENS, TOP_K).astype(jnp.int32)


def levels(key, extent, cuts, low, high):
    gain = 1.0
    for dim, blocks in cuts:
        steps = jax.random.uniform(jax.random.fold_in(jax.random.fold_in(key, 6), dim), (blocks,), jnp.float32, low / len(cuts), high / len(cuts))
        gain = gain * jnp.repeat(jnp.exp(steps), extent[dim] // blocks).reshape((-1,) + (1,) * (len(extent) - 1 - dim))
    return gain


def bell_draw(own_key, dims, scale, bound, shards=(), held_as=jnp.bfloat16):
    result = scale * jax.random.normal(own_key, dims, jnp.float32)
    if shards:
        result = result * levels(own_key, dims, shards, -0.22, 0.18)
    return jnp.clip(result, -bound, bound).astype(held_as)


def setup_inputs(seed: int = 0) -> dict:
    splits = jax.random.split(jax.random.key(seed), 11)
    return {
        "tokens": bell_draw(splits[0], (TOKENS, D), 1.0, 6.0, ((0, 128),)),
        "norm_gain": jnp.clip(1.0 + 0.18 * jax.random.normal(splits[1], (D,), jnp.float32), 0.1, 1.9),
        "expert_ids": draw_expert_ids(jax.random.fold_in(splits[10], 71), 0),
        "gate_weights": jnp.clip(0.1 + 0.5 * jax.random.uniform(splits[3], (TOKENS, TOP_K), jnp.float32) ** levels(splits[3], (TOKENS, TOP_K), ((0, 128),), -0.2, 0.2), 0.1, 0.6),
        "expert_gate": bell_draw(splits[4], (EXPERTS, D, DE), D ** -0.5, 0.125, ((0, 128),)),
        "expert_up": bell_draw(splits[5], (EXPERTS, D, DE), D ** -0.5, 0.125, ((0, 128),)),
        "expert_down": bell_draw(splits[6], (EXPERTS, DE, D), DE ** -0.5, 0.25, ((0, 128),)),
        "shared_gate": bell_draw(splits[7], (D, DS), D ** -0.5, 0.125, ((0, 128),)),
        "shared_up": bell_draw(splits[8], (D, DS), D ** -0.5, 0.125, ((0, 128),)),
        "shared_down": bell_draw(splits[9], (DS, D), DS ** -0.5, 0.25, ((1, 128),)),
    }


EPS = 1e-06

def normalize(tokens, norm_gain):
    values = tokens.astype(jnp.float32)
    scaled = values * lax.rsqrt(lax.optimization_barrier(jnp.mean(values * values, axis=-1, keepdims=True)) + EPS)
    return (scaled * norm_gain.astype(jnp.float32)).astype(jnp.bfloat16)

def swiglu(inputs, w_gate, w_up, w_down):
    gate_val = jnp.dot(inputs, w_gate, preferred_element_type=jnp.float32)
    up_val = jnp.dot(inputs, w_up, preferred_element_type=jnp.float32)
    hidden = (jax.nn.silu(gate_val) * up_val).astype(jnp.bfloat16)
    return jnp.dot(hidden, w_down, preferred_element_type=jnp.float32)

def reference(tokens, norm_gain, expert_ids, gate_weights, expert_gate, expert_up, expert_down, shared_gate, shared_up, shared_down):
    normed = normalize(tokens, norm_gain)
    count_tok = normed.shape[0]
    width = normed.shape[1]
    assign = count_tok * TOP_K
    flat_ids = expert_ids.reshape(assign).astype(jnp.int32)
    ordering = jnp.argsort(flat_ids, stable=True).astype(jnp.int32)
    sorted_ids = flat_ids[ordering]
    sorted_tok = (ordering // TOP_K).astype(jnp.int32)
    sorted_wts = gate_weights.reshape(assign)[ordering]
    counts = jnp.bincount(flat_ids, length=EXPERTS).astype(jnp.int32)
    block_rows = 256
    padded = ((counts + block_rows - 1) // block_rows * block_rows).astype(jnp.int32)
    pad_end = jnp.cumsum(padded).astype(jnp.int32)
    pad_start = pad_end - padded
    cnt_start = (jnp.cumsum(counts).astype(jnp.int32) - counts).astype(jnp.int32)
    dest = (pad_start[sorted_ids] + jnp.arange(assign, dtype=jnp.int32) - cnt_start[sorted_ids]).astype(jnp.int32)
    blocks = -(-(assign + EXPERTS * (block_rows - 1)) // block_rows)
    total_rows = blocks * block_rows
    row_tok = jnp.full((total_rows,), count_tok, jnp.int32).at[dest].set(sorted_tok)
    row_wts = jnp.zeros((total_rows,), jnp.float32).at[dest].set(sorted_wts)
    block_expert = jnp.minimum(jnp.searchsorted(pad_end, jnp.arange(blocks, dtype=jnp.int32) * block_rows, side='right'), EXPERTS - 1).astype(jnp.int32)
    padded_x = jnp.concatenate([normed, jnp.zeros((1, width), jnp.bfloat16)], axis=0)

    def step(accum, inputs_blk):
        tok_blk, wts_blk, expert = inputs_blk
        picked = padded_x[tok_blk]
        output = swiglu(picked, expert_gate[expert], expert_up[expert], expert_down[expert]).astype(jnp.bfloat16)
        accum = accum.at[tok_blk].add(output.astype(jnp.float32) * wts_blk[:, None])
        return (accum, None)
    routed, _ = lax.scan(step, jnp.zeros((count_tok + 1, width), jnp.float32), (row_tok.reshape(blocks, block_rows), row_wts.reshape(blocks, block_rows), block_expert))
    shared = swiglu(normed, shared_gate, shared_up, shared_down)
    return (routed[:count_tok] + shared).astype(jnp.bfloat16)
```

```python
import jax
import jax.numpy as jnp
from jax import lax
from jax.experimental import pallas as pl
from jax.experimental.pallas import tpu as pltpu
from jax.sharding import PartitionSpec as P

EPS = 1e-06
MESH = pl.DeviceIdType.MESH
F32, BF16 = jnp.float32, jnp.bfloat16

D = 2048
DE = 512
NJ = 4
F = D // NJ
LINE = 4
TOK = 128
CAP = 6
BLK = LINE * CAP
PEERS = 32
ROWS = PEERS * BLK
COLS = LINE * TOK
HS = 128
SLAB = 16

_CHIP = [(0, 1), (1, 0), (0, 3), (3, 0), (1, 1), (1, 3), (3, 1), (3, 3), (0, 2), (2, 0), (2, 1), (1, 2), (2, 3), (3, 2), (2, 2)]
PLANE = [(a, b, 0) for a, b in _CHIP] + [(0, 0, 1)] + [(a, b, 1) for a, b in _CHIP]
LINEK = (1, 3, 2)


def silu(v):
    return v / (1.0 + jnp.exp(-v))


def dot(a, b):
    return jnp.dot(a, b, preferred_element_type=F32)


def dot_t(a, b):
    return lax.dot_general(a, b, (((1,), (1,)), ((), ())), preferred_element_type=F32)


def row_pattern(shape, dim, offset):
    row = (lax.broadcasted_iota(jnp.int32, shape, dim) + offset).astype(F32)
    peer = jnp.floor((row + 0.5) * (1.0 / BLK))
    inner = row - BLK * peer
    line = jnp.floor((inner + 0.5) * (1.0 / CAP))
    slot = inner - CAP * line
    return peer, inner, 8.0 * line + slot + 1.0


def kernel(
    tok, gain, ids, gw, sg, su, sd, wg_hbm, wu_hbm, wd_hbm, out,
    wgu, wd, x4, meta, sown, sgather, wsg, wsu, wsd, vmat, bits, sel, wsel, lab_out, lab_in,
    send, got, gu, hid, back, ret, hs, part, parts,
    wsem, msem, ssem, xsem, lsem, dsem, rsem, psem,
):
    me = lax.axis_index("ep")
    z, y, x, c = lax.div(me, 32), lax.rem(lax.div(me, 8), 4), lax.rem(lax.div(me, 2), 4), lax.rem(me, 2)
    mine = lax.rem(me, 32)
    sends = []

    def remote(src, dst, landed, sems, at, dev, start=True):
        s, r = sems.at[(0,) + at], sems.at[(1,) + at]
        go = pltpu.make_async_remote_copy(src, dst, s, r, device_id=(dev,), device_id_type=MESH)
        go.start()
        sends.append(go)
        return pltpu.make_async_remote_copy(src, landed, s, r, device_id=(dev,), device_id_type=MESH)

    def on_z(k):
        return lax.rem(z + k, 4), lax.rem(z + 4 - k, 4)

    def zdev(zz):
        return zz * 32 + mine

    plane = []
    for dy, dx, dc in PLANE:
        to = lax.rem(y + dy, 4) * 8 + lax.rem(x + dx, 4) * 2 + lax.rem(c + dc, 2)
        frm = lax.rem(y + 4 - dy, 4) * 8 + lax.rem(x + 4 - dx, 4) * 2 + lax.rem(c + dc, 2)
        plane.append((to, frm, z * 32 + to))

    def rows_of(b):
        return pl.ds(pl.multiple_of(b * BLK, 8), BLK)

    def toks_of(zz):
        return pl.ds(pl.multiple_of(zz * TOK, TOK), TOK)

    barrier = pltpu.get_barrier_semaphore()
    for k in LINEK:
        pl.semaphore_signal(barrier, inc=1, device_id=(zdev(on_z(k)[0]),), device_id_type=MESH)
    for _, _, dev in plane:
        pl.semaphore_signal(barrier, inc=1, device_id=(dev,), device_id_type=MESH)

    weights = []
    for e in range(2):
        weights.append(pltpu.make_async_copy(wg_hbm.at[e], wgu.at[2 * e], wsem.at[3 * e]))
        weights.append(pltpu.make_async_copy(wu_hbm.at[e], wgu.at[2 * e + 1], wsem.at[3 * e + 1]))
    for e in range(2):
        weights.append(pltpu.make_async_copy(wd_hbm.at[e], wd.at[pl.ds(e * DE, DE)], wsem.at[3 * e + 2]))
    for w in weights:
        w.start()

    meta[z, 0:4, :] = ids[...].astype(F32)
    meta[z, 4:8, :] = gw[...]

    def norm_tile(i, carry):
        r = pl.ds(pl.multiple_of(i * 16, 16), 16)
        t = tok[r, :].astype(F32)
        t = t * lax.rsqrt(jnp.mean(t * t, axis=-1, keepdims=True) + EPS)
        t = (t * gain[...]).astype(BF16)
        at = pl.ds(pl.multiple_of(z * TOK + i * 16, 16), 16)
        for j in range(NJ):
            x4[j, at, :] = t[:, j * F:(j + 1) * F]
        return carry

    lax.fori_loop(0, TOK // 16, norm_tile, 0)
    for q in range(4):
        cut = slice(q * HS, (q + 1) * HS)
        sown[q, 0:SLAB, :] = sg[:, cut]
        sown[q, SLAB:2 * SLAB, :] = su[:, cut]
        sown[q, 2 * SLAB:3 * SLAB, :] = sd[:, cut]
    sgather[c, x, y, z] = sown[z]

    pl.semaphore_wait(barrier, len(LINEK) + len(PLANE))

    meta_in, slab_z, x_in = [], [], [[] for _ in range(NJ)]
    for k in LINEK:
        to, frm = on_z(k)
        meta_in.append(remote(meta.at[z], meta.at[z], meta.at[frm], msem, (k - 1,), zdev(to)))

    def send_x(j):
        for k in LINEK:
            to, frm = on_z(k)
            x_in[j].append(remote(x4.at[j, toks_of(z)], x4.at[j, toks_of(z)], x4.at[j, toks_of(frm)], xsem, (j, k - 1), zdev(to)))

    send_x(0)
    for k in LINEK:
        to, frm = on_z(k)
        slab_z.append(remote(sown.at[to], sgather.at[c, x, y, z], sgather.at[c, x, y, frm], ssem, (k - 1,), zdev(to)))
    for j in range(1, NJ):
        send_x(j)

    for m in meta_in:
        m.wait_recv()
    here = lax.broadcasted_iota(jnp.int32, (PEERS, TOK), 0).astype(F32) + (z * PEERS).astype(F32)
    before = (
        lax.broadcasted_iota(jnp.int32, (TOK, TOK), 0) < lax.broadcasted_iota(jnp.int32, (TOK, TOK), 1)
    ).astype(F32).astype(BF16)
    wvals, slots, whichs = [], [], []
    for q in range(LINE):
        hit = jnp.zeros((PEERS, TOK), F32)
        wv = jnp.zeros((PEERS, TOK), F32)
        bit = jnp.zeros((PEERS, TOK), F32)
        for k in range(4):
            e = meta[q, k:k + 1, :]
            dev = jnp.floor(e * 0.5)
            is_k = (here == dev).astype(F32)
            hit = hit + is_k
            wv = wv + is_k * meta[q, 4 + k:5 + k, :]
            bit = bit + is_k * (e - 2.0 * dev)
        rank = dot(hit.astype(BF16), before)
        slots.append(jnp.where(hit > 0.0, rank + (8.0 * q + 1.0), 0.0))
        wvals.append(wv)
        whichs.append(bit)
    lane = lax.broadcasted_iota(jnp.int32, (PEERS, 128), 1)
    labels = jnp.zeros((PEERS, 128), F32)
    for q in range(LINE):
        for s in range(CAP):
            bit = jnp.sum(jnp.where(slots[q] == 8.0 * q + s + 1.0, whichs[q], 0.0), axis=1, keepdims=True)
            labels = jnp.where(lane == q * CAP + s, bit, labels)
    for b in range(PEERS):
        lab_out[b] = labels[b:b + 1, :]
    lab_in[mine] = lab_out[mine]

    pad = jnp.zeros((128 - PEERS, TOK), F32)
    for q in range(LINE):
        cut = slice(q * TOK, (q + 1) * TOK)
        vmat[0, :, cut] = jnp.concatenate([slots[q], pad], axis=0).astype(BF16)
        bits[0, cut, :] = jnp.transpose(jnp.concatenate([slots[q], pad], axis=0)).astype(BF16)
        bits[1, cut, :] = jnp.transpose(jnp.concatenate([wvals[q], pad], axis=0)).astype(BF16)

    def sel_tile(i, carry):
        peer, _, target = row_pattern((128, 128), 0, i * 128)
        pick = (peer == lax.broadcasted_iota(jnp.int32, (128, 128), 1).astype(F32)).astype(F32).astype(BF16)
        val = dot(pick, vmat[0])
        sel[pl.ds(pl.multiple_of(i * 128, 128), 128), :] = (val == target[:, 0:1]).astype(F32).astype(BF16)
        return carry

    lax.fori_loop(0, ROWS // 128, sel_tile, 0)

    def dispatch(j):
        for n in range(F // 256):
            cut = slice(n * 256, (n + 1) * 256)
            send[j, :, cut] = dot(sel[...], x4[j, :, cut]).astype(BF16)
        arrivals = []
        for i, (to, frm, dev) in enumerate(plane):
            arrivals.append(remote(send.at[j, rows_of(to)], got.at[j, rows_of(mine)], got.at[j, rows_of(frm)], dsem, (j, i), dev))
        got[j, rows_of(mine), :] = send[j, rows_of(mine), :]
        return arrivals

    got_in = []
    for m in x_in[0]:
        m.wait_recv()
    got_in.append(dispatch(0))
    label_in = [
        remote(lab_out.at[to], lab_in.at[mine], lab_in.at[frm], lsem, (i,), dev)
        for i, (to, frm, dev) in enumerate(plane)
    ]
    for m in slab_z:
        m.wait_recv()
    slab_y = []
    for k in LINEK:
        to, frm = lax.rem(y + k, 4), lax.rem(y + 4 - k, 4)
        slab_y.append(remote(sgather.at[c, x, y], sgather.at[c, x, y], sgather.at[c, x, frm], ssem, (2 + k,), z * 32 + to * 8 + x * 2 + c))
    for m in x_in[1]:
        m.wait_recv()
    got_in.append(dispatch(1))
    for m in slab_y:
        m.wait_recv()
    slab_x = []
    for k in LINEK:
        to, frm = lax.rem(x + k, 4), lax.rem(x + 4 - k, 4)
        slab_x.append(remote(sgather.at[c, x], sgather.at[c, x], sgather.at[c, frm], ssem, (5 + k,), z * 32 + y * 8 + to * 2 + c))
    for j in range(2, NJ):
        for m in x_in[j]:
            m.wait_recv()
        got_in.append(dispatch(j))

    def wsel_tile(i, carry):
        peer, _, target = row_pattern((128, 128), 1, i * 128)
        pick = (peer == lax.broadcasted_iota(jnp.int32, (128, 128), 0).astype(F32)).astype(F32).astype(BF16)
        val = dot(bits[0], pick)
        w = dot(bits[1], pick)
        wsel[:, pl.ds(pl.multiple_of(i * 128, 128), 128)] = jnp.where(val == target[0:1, :], w, 0.0).astype(BF16)
        return carry

    lax.fori_loop(0, ROWS // 128, wsel_tile, 0)

    for m in slab_x:
        m.wait_recv()
    slab_c = remote(sgather.at[c], sgather.at[c], sgather.at[1 - c], ssem, (9,), z * 32 + y * 8 + x * 2 + 1 - c)

    for m in label_in:
        m.wait_recv()
    for w in weights:
        w.wait()

    vmat[1] = jnp.zeros((128, COLS), BF16)
    for b in range(PEERS):
        bits[2, b:b + 1, :] = lab_in[b].astype(BF16)

    for j in range(NJ - 1):
        for m in got_in[j]:
            m.wait_recv()

        def accumulate(n, carry, j=j):
            q = lax.div(n, 2)
            cut = pl.ds(pl.multiple_of(lax.rem(n, 2) * 256, 256), 256)
            prod = dot(got[j], wgu[q, j * F:(j + 1) * F, cut])
            if j == 0:
                gu[q, :, cut] = prod
            else:
                gu[q, :, cut] += prod
            return carry

        lax.fori_loop(0, 8, accumulate, 0)

    peer, inner, _ = row_pattern((ROWS, 128), 0, 0)
    lane = lax.broadcasted_iota(jnp.int32, (ROWS, 128), 1).astype(F32)
    pick = (peer == lane).astype(F32)
    lab = dot(pick.astype(BF16)[:, 0:PEERS], bits[2, 0:PEERS, :])
    which = jnp.sum(jnp.where(inner == lane, lab, 0.0), axis=1, keepdims=True)

    j = NJ - 1
    for m in got_in[j]:
        m.wait_recv()
    for e in range(2):
        keep = which if e == 1 else 1.0 - which
        for n in range(2):
            cut = slice(n * 256, (n + 1) * 256)
            g = gu[2 * e, :, cut] + dot(got[j], wgu[2 * e, j * F:(j + 1) * F, cut])
            u = gu[2 * e + 1, :, cut] + dot(got[j], wgu[2 * e + 1, j * F:(j + 1) * F, cut])
            hid[:, e * DE + n * 256:e * DE + (n + 1) * 256] = (silu(g) * u * keep).astype(BF16)

    ret_in = []
    for j in range(NJ):
        for n in range(F // 256):
            back[j, :, n * 256:(n + 1) * 256] = dot(hid[...], wd[:, j * F + n * 256:j * F + (n + 1) * 256]).astype(BF16)
        arrivals = []
        for i, (to, frm, dev) in enumerate(plane):
            arrivals.append(remote(back.at[j, rows_of(to)], ret.at[j, rows_of(mine)], ret.at[j, rows_of(frm)], rsem, (j, i), dev))
        ret[j, rows_of(mine), :] = back[j, rows_of(mine), :]
        ret_in.append(arrivals)

    slab_c.wait_recv()
    for zz in range(4):
        for yy in range(4):
            for xx in range(4):
                for cc in range(2):
                    r = (((zz * 4 + yy) * 4 + xx) * 2 + cc) * SLAB
                    wsg[r:r + SLAB, :] = sgather[cc, xx, yy, zz, 0:SLAB, :]
                    wsu[r:r + SLAB, :] = sgather[cc, xx, yy, zz, SLAB:2 * SLAB, :]
                    wsd[r:r + SLAB, :] = sgather[cc, xx, yy, zz, 2 * SLAB:3 * SLAB, :]
    g = jnp.zeros((COLS, HS), F32)
    u = jnp.zeros((COLS, HS), F32)
    for j in range(NJ):
        g = g + dot(x4[j], wsg[j * F:(j + 1) * F, :])
        u = u + dot(x4[j], wsu[j * F:(j + 1) * F, :])
    hs[...] = (silu(g) * u).astype(BF16)

    part_in = []
    for j in range(NJ):
        for m in ret_in[j]:
            m.wait_recv()
        for n in range(F // 256):
            at = j * F + n * 256
            val = dot(wsel[...], ret[j, :, n * 256:(n + 1) * 256]) + dot_t(hs[...], wsd[at:at + 256, :])
            part[j, :, n * 256:(n + 1) * 256] = val.astype(BF16)
        arrivals = []
        for k in LINEK:
            to, frm = on_z(k)
            arrivals.append(remote(part.at[j, toks_of(to)], parts.at[j, toks_of(z)], parts.at[j, toks_of(frm)], psem, (j, k - 1), zdev(to)))
        parts[j, toks_of(z), :] = part[j, toks_of(z), :]
        part_in.append(arrivals)

    for j in range(NJ):
        for m in part_in[j]:
            m.wait_recv()
        total = parts[j, 0:TOK, :].astype(F32)
        for q in range(1, LINE):
            total = total + parts[j, q * TOK:(q + 1) * TOK, :].astype(F32)
        out[:, j * F:(j + 1) * F] = total.astype(BF16)

    for s in sends:
        s.wait_send()


def per_device(tokens, norm_gain, expert_ids, gate_weights, expert_gate, expert_up, expert_down, shared_gate, shared_up, shared_down):
    vmem = pl.BlockSpec(memory_space=pltpu.VMEM)
    hbm = pl.BlockSpec(memory_space=pl.ANY)
    dma = pltpu.SemaphoreType.DMA
    n = len(PLANE)
    return pl.pallas_call(
        kernel,
        out_shape=jax.ShapeDtypeStruct((TOK, D), BF16),
        in_specs=[vmem] * 7 + [hbm] * 3,
        out_specs=vmem,
        scratch_shapes=[
            pltpu.VMEM((4, D, DE), BF16),
            pltpu.VMEM((2 * DE, D), BF16),
            pltpu.VMEM((NJ, COLS, F), BF16),
            pltpu.VMEM((LINE, 8, TOK), F32),
            pltpu.VMEM((4, 3 * SLAB, HS), BF16),
            pltpu.VMEM((2, 4, 4, 4, 3 * SLAB, HS), BF16),
            pltpu.VMEM((D, HS), BF16),
            pltpu.VMEM((D, HS), BF16),
            pltpu.VMEM((D, HS), BF16),
            pltpu.VMEM((2, 128, COLS), BF16),
            pltpu.VMEM((3, COLS, 128), BF16),
            pltpu.VMEM((ROWS, COLS), BF16),
            pltpu.VMEM((COLS, ROWS), BF16),
            pltpu.VMEM((PEERS, 1, 128), F32),
            pltpu.VMEM((PEERS, 1, 128), F32),
            pltpu.VMEM((NJ, ROWS, F), BF16),
            pltpu.VMEM((NJ, ROWS, F), BF16),
            pltpu.VMEM((4, ROWS, DE), F32),
            pltpu.VMEM((ROWS, 2 * DE), BF16),
            pltpu.VMEM((NJ, ROWS, F), BF16),
            pltpu.VMEM((NJ, ROWS, F), BF16),
            pltpu.VMEM((COLS, HS), BF16),
            pltpu.VMEM((NJ, COLS, F), BF16),
            pltpu.VMEM((NJ, COLS, F), BF16),
            dma((6,)),
            dma((2, 3)),
            dma((2, 10)),
            dma((2, NJ, 3)),
            dma((2, n)),
            dma((2, NJ, n)),
            dma((2, NJ, n)),
            dma((2, NJ, 3)),
        ],
        compiler_params=pltpu.CompilerParams(
            collective_id=0, has_side_effects=True, vmem_limit_bytes=67043328
        ),
        name="moe",
    )(
        tokens, norm_gain.reshape(1, D), expert_ids.T, gate_weights.T,
        shared_gate, shared_up, shared_down.T, expert_gate, expert_up, expert_down,
    )


def solution(mesh):
    ep = P("ep")
    return jax.shard_map(
        per_device,
        mesh=mesh,
        in_specs=(ep, P(), ep, ep, ep, ep, ep, ep, ep, P(None, "ep")),
        out_specs=ep,
        check_vma=False,
    )
```

```python
import jax
import jax.numpy as jnp
from jax import lax
from jax.experimental import pallas as pl
from jax.experimental.pallas import tpu as pltpu
from jax.sharding import PartitionSpec as P

EPS = 1e-06
MESH = pl.DeviceIdType.MESH
F32, BF16 = jnp.float32, jnp.bfloat16

D = 2048
DE = 512
F = 256
NS = D // F
GROUPS = [(0, 1), (1, 3), (3, 5), (5, 7), (7, 8)]
NG = len(GROUPS)
LINE = 4
TOK = 128
CAP = 6
BLK = LINE * CAP
PEERS = 32
ROWS = PEERS * BLK
COLS = LINE * TOK
HS = 128
SLAB = 16

_CHIP = [(0, 1), (1, 0), (0, 3), (3, 0), (1, 1), (1, 3), (3, 1), (3, 3), (0, 2), (2, 0), (2, 1), (1, 2), (2, 3), (3, 2), (2, 2)]
PLANE = [(a, b, 0) for a, b in _CHIP] + [(0, 0, 1)] + [(a, b, 1) for a, b in _CHIP]
LINEK = (1, 3, 2)


def silu(v):
    return v / (1.0 + jnp.exp(-v))


def dot(a, b):
    return jnp.dot(a, b, preferred_element_type=F32)


def dot_t(a, b):
    return lax.dot_general(a, b, (((1,), (1,)), ((), ())), preferred_element_type=F32)


def row_pattern(shape, dim, offset):
    row = (lax.broadcasted_iota(jnp.int32, shape, dim) + offset).astype(F32)
    peer = jnp.floor((row + 0.5) * (1.0 / BLK))
    inner = row - BLK * peer
    line = jnp.floor((inner + 0.5) * (1.0 / CAP))
    slot = inner - CAP * line
    return peer, inner, 8.0 * line + slot + 1.0


def kernel(
    tok_hbm, gain_hbm, ids_hbm, gw_hbm, sg_hbm, su_hbm, sd_hbm, wg_hbm, wu_hbm, wd_hbm, out_hbm,
    tok, gain, ids, gw, sg, su, sd,
    wgu, wd, x4, meta, sown, sgather, wsg, wsu, wsd, vmat, bits, sel, wsel, lab_out, lab_in,
    send, got, gu, hid, back, ret, hs, part, parts, out,
    isem, wsem, osem, msem, ssem, xsem, lsem, dsem, rsem, psem,
):
    me = lax.axis_index("ep")
    z, y, x, c = lax.div(me, 32), lax.rem(lax.div(me, 8), 4), lax.rem(lax.div(me, 2), 4), lax.rem(me, 2)
    mine = lax.rem(me, 32)
    sends = []

    def copy_to(src, dst, sems, at, dev):
        return pltpu.make_async_remote_copy(src, dst, sems.at[(0,) + at], sems.at[(1,) + at], device_id=(dev,), device_id_type=MESH)

    def remote(src, dst, landed, sems, at, dev):
        go = copy_to(src, dst, sems, at, dev)
        go.start()
        sends.append(go)
        return copy_to(src, landed, sems, at, dev)

    def line(v, k):
        return lax.rem(v + k, 4), lax.rem(v + 4 - k, 4)

    def zdev(zz):
        return zz * 32 + mine

    def pdev(yy, xx, cc):
        return z * 32 + yy * 8 + xx * 2 + cc

    plane = []
    for dy, dx, dc in PLANE:
        to = lax.rem(y + dy, 4) * 8 + lax.rem(x + dx, 4) * 2 + lax.rem(c + dc, 2)
        plane.append((to, z * 32 + to))

    def rows_of(b):
        return pl.ds(pl.multiple_of(b * BLK, 8), BLK)

    def toks_of(zz):
        return pl.ds(pl.multiple_of(zz * TOK, TOK), TOK)

    def exchange(src, dst, group, sems):
        a, b = GROUPS[group]
        for to, dev in plane:
            copy_to(src.at[a:b, rows_of(to)], dst.at[a:b, rows_of(mine)], sems, (group,), dev).start()
        for q in range(a, b):
            dst[q, rows_of(mine), :] = src[q, rows_of(mine), :]
        every = pl.ds(0, len(plane) * BLK)
        done = copy_to(src.at[a:b, every], dst.at[a:b, every], sems, (group,), plane[0][1])
        sends.append(done)
        return done

    small = [
        pltpu.make_async_copy(src, dst, isem.at[i])
        for i, (src, dst) in enumerate(
            [(tok_hbm, tok), (gain_hbm, gain), (ids_hbm, ids), (gw_hbm, gw), (sg_hbm, sg), (su_hbm, su), (sd_hbm, sd)]
        )
    ]
    for m in small:
        m.start()

    barrier = pltpu.get_barrier_semaphore()
    for k in LINEK:
        pl.semaphore_signal(barrier, inc=1, device_id=(zdev(line(z, k)[0]),), device_id_type=MESH)
    for _, dev in plane:
        pl.semaphore_signal(barrier, inc=1, device_id=(dev,), device_id_type=MESH)

    weights = []
    for e in range(2):
        weights.append(pltpu.make_async_copy(wg_hbm.at[e], wgu.at[2 * e], wsem.at[3 * e]))
        weights.append(pltpu.make_async_copy(wu_hbm.at[e], wgu.at[2 * e + 1], wsem.at[3 * e + 1]))
    for e in range(2):
        weights.append(pltpu.make_async_copy(wd_hbm.at[e], wd.at[pl.ds(e * DE, DE)], wsem.at[3 * e + 2]))
    for m in small:
        m.wait()
    for w in weights:
        w.start()

    meta[z, 0:4, :] = ids[...].astype(F32)
    meta[z, 4:8, :] = gw[...]
    for q in range(4):
        cut = slice(q * HS, (q + 1) * HS)
        sown[q, 0:SLAB, :] = sg[:, cut]
        sown[q, SLAB:2 * SLAB, :] = su[:, cut]
        sown[q, 2 * SLAB:3 * SLAB, :] = sd[:, cut]
    sgather[c, x, y, z] = sown[z]

    def norm_tile(i, carry):
        r = pl.ds(pl.multiple_of(i * 16, 16), 16)
        t = tok[r, :].astype(F32)
        t = t * lax.rsqrt(jnp.mean(t * t, axis=-1, keepdims=True) + EPS)
        t = (t * gain[...]).astype(BF16)
        at = pl.ds(pl.multiple_of(z * TOK + i * 16, 16), 16)
        for q in range(NS):
            x4[q, at, :] = t[:, q * F:(q + 1) * F]
        return carry

    lax.fori_loop(0, TOK // 16, norm_tile, 0)

    pl.semaphore_wait(barrier, len(LINEK) + len(PLANE))

    meta_in, slab_z, x_in = [], [], [[] for _ in range(NG)]
    for k in LINEK:
        to, frm = line(z, k)
        slab_z.append(remote(sown.at[to], sgather.at[c, x, y, z], sgather.at[c, x, y, frm], ssem, (k - 1,), zdev(to)))
    for k in LINEK:
        to, frm = line(z, k)
        meta_in.append(remote(meta.at[z], meta.at[z], meta.at[frm], msem, (k - 1,), zdev(to)))
    for g, (a, b) in enumerate(GROUPS):
        for k in LINEK:
            to, frm = line(z, k)
            x_in[g].append(remote(x4.at[a:b, toks_of(z)], x4.at[a:b, toks_of(z)], x4.at[a:b, toks_of(frm)], xsem, (g, k - 1), zdev(to)))

    half = 3 * SLAB // 2
    top, low = pl.ds(0, half), pl.ds(half, half)
    for m in slab_z:
        m.wait_recv()
    slab_1, slab_2 = [], []
    for k in LINEK:
        to, frm = line(y, k)
        slab_1.append(remote(sgather.at[c, x, y, :, top], sgather.at[c, x, y, :, top], sgather.at[c, x, frm, :, top], ssem, (2 + k,), pdev(to, x, c)))
        to, frm = line(x, k)
        slab_1.append(remote(sgather.at[c, x, y, :, low], sgather.at[c, x, y, :, low], sgather.at[c, frm, y, :, low], ssem, (5 + k,), pdev(y, to, c)))

    for m in meta_in:
        m.wait_recv()
    here = lax.broadcasted_iota(jnp.int32, (PEERS, TOK), 0).astype(F32) + (z * PEERS).astype(F32)
    before = (
        lax.broadcasted_iota(jnp.int32, (TOK, TOK), 0) < lax.broadcasted_iota(jnp.int32, (TOK, TOK), 1)
    ).astype(F32).astype(BF16)
    wvals, slots, whichs = [], [], []
    for q in range(LINE):
        hit = jnp.zeros((PEERS, TOK), F32)
        wv = jnp.zeros((PEERS, TOK), F32)
        bit = jnp.zeros((PEERS, TOK), F32)
        for k in range(4):
            e = meta[q, k:k + 1, :]
            dev = jnp.floor(e * 0.5)
            is_k = (here == dev).astype(F32)
            hit = hit + is_k
            wv = wv + is_k * meta[q, 4 + k:5 + k, :]
            bit = bit + is_k * (e - 2.0 * dev)
        rank = dot(hit.astype(BF16), before)
        slots.append(jnp.where(hit > 0.0, rank + (8.0 * q + 1.0), 0.0))
        wvals.append(wv)
        whichs.append(bit)

    pad = jnp.zeros((128 - PEERS, TOK), F32)
    for q in range(LINE):
        cut = slice(q * TOK, (q + 1) * TOK)
        vmat[:, cut] = jnp.concatenate([slots[q], pad], axis=0).astype(BF16)

    def sel_tile(i, carry):
        peer, _, target = row_pattern((128, 128), 0, i * 128)
        pick = (peer == lax.broadcasted_iota(jnp.int32, (128, 128), 1).astype(F32)).astype(F32).astype(BF16)
        val = dot(pick, vmat[...])
        sel[pl.ds(pl.multiple_of(i * 128, 128), 128), :] = (val == target[:, 0:1]).astype(F32).astype(BF16)
        return carry

    lax.fori_loop(0, ROWS // 128, sel_tile, 0)

    for m in slab_1:
        m.wait_recv()
    for k in LINEK:
        to, frm = line(x, k)
        slab_2.append(remote(sgather.at[c, x, :, :, top], sgather.at[c, x, :, :, top], sgather.at[c, frm, :, :, top], ssem, (8 + k,), pdev(y, to, c)))
        to, frm = line(y, k)
        slab_2.append(remote(sgather.at[c, :, y, :, low], sgather.at[c, :, y, :, low], sgather.at[c, :, frm, :, low], ssem, (11 + k,), pdev(to, x, c)))

    def dispatch(g):
        for m in x_in[g]:
            m.wait_recv()
        for q in range(*GROUPS[g]):
            send[q] = dot(sel[...], x4[q]).astype(BF16)
        return exchange(send, got, g, dsem)

    got_in = [dispatch(0)]

    lane = lax.broadcasted_iota(jnp.int32, (PEERS, 128), 1)
    labels = jnp.zeros((PEERS, 128), F32)
    for q in range(LINE):
        for s in range(CAP):
            bit = jnp.sum(jnp.where(slots[q] == 8.0 * q + s + 1.0, whichs[q], 0.0), axis=1, keepdims=True)
            labels = jnp.where(lane == q * CAP + s, bit, labels)
    for b in range(PEERS):
        lab_out[b] = labels[b:b + 1, :]
    lab_in[mine] = lab_out[mine]
    for to, dev in plane:
        copy_to(lab_out.at[to], lab_in.at[mine], lsem, (), dev).start()
    every = pl.ds(0, len(plane))
    label_in = copy_to(lab_out.at[every], lab_in.at[every], lsem, (), plane[0][1])
    sends.append(label_in)
    for q in range(LINE):
        cut = slice(q * TOK, (q + 1) * TOK)
        bits[0, cut, :] = jnp.transpose(jnp.concatenate([slots[q], pad], axis=0)).astype(BF16)
        bits[1, cut, :] = jnp.transpose(jnp.concatenate([wvals[q], pad], axis=0)).astype(BF16)

    got_in.append(dispatch(1))
    for m in slab_2:
        m.wait_recv()
    slab_c = remote(sgather.at[c], sgather.at[c], sgather.at[1 - c], ssem, (15,), pdev(y, x, 1 - c))
    for g in range(2, NG):
        got_in.append(dispatch(g))

    def wsel_tile(i, carry):
        peer, _, target = row_pattern((128, 128), 1, i * 128)
        pick = (peer == lax.broadcasted_iota(jnp.int32, (128, 128), 0).astype(F32)).astype(F32).astype(BF16)
        val = dot(bits[0], pick)
        w = dot(bits[1], pick)
        wsel[:, pl.ds(pl.multiple_of(i * 128, 128), 128)] = jnp.where(val == target[0:1, :], w, 0.0).astype(BF16)
        return carry

    lax.fori_loop(0, ROWS // 128, wsel_tile, 0)

    for w in weights:
        w.wait()
    label_in.wait_recv()
    for b in range(PEERS):
        bits[2, b:b + 1, :] = lab_in[b].astype(BF16)
    peer, inner, _ = row_pattern((ROWS, 128), 0, 0)
    lane = lax.broadcasted_iota(jnp.int32, (ROWS, 128), 1).astype(F32)
    pick = (peer == lane).astype(F32)
    lab = dot(pick.astype(BF16)[:, 0:PEERS], bits[2, 0:PEERS, :])
    which = jnp.sum(jnp.where(inner == lane, lab, 0.0), axis=1, keepdims=True)

    def partial(group, q, cut):
        return sum(dot(got[s], wgu[q, s * F:(s + 1) * F, cut]) for s in range(*GROUPS[group]))

    for g in range(NG - 1):
        got_in[g].wait_recv()

        def accumulate(n, carry, g=g):
            q = lax.div(n, 2)
            cut = pl.ds(pl.multiple_of(lax.rem(n, 2) * 256, 256), 256)
            prod = partial(g, q, cut)
            if g == 0:
                gu[q, :, cut] = prod
            else:
                gu[q, :, cut] += prod
            return carry

        lax.fori_loop(0, 8, accumulate, 0)

    got_in[NG - 1].wait_recv()
    for e in range(2):
        keep = which if e == 1 else 1.0 - which
        for n in range(2):
            cut = slice(n * 256, (n + 1) * 256)
            g = gu[2 * e, :, cut] + partial(NG - 1, 2 * e, cut)
            u = gu[2 * e + 1, :, cut] + partial(NG - 1, 2 * e + 1, cut)
            hid[:, e * DE + n * 256:e * DE + (n + 1) * 256] = (silu(g) * u * keep).astype(BF16)

    ret_in = []
    for g in range(NG):
        for q in range(*GROUPS[g]):
            back[q] = dot(hid[...], wd[:, q * F:(q + 1) * F]).astype(BF16)
        ret_in.append(exchange(back, ret, g, rsem))

    slab_c.wait_recv()
    for zz in range(4):
        for yy in range(4):
            for xx in range(4):
                for cc in range(2):
                    r = (((zz * 4 + yy) * 4 + xx) * 2 + cc) * SLAB
                    wsg[r:r + SLAB, :] = sgather[cc, xx, yy, zz, 0:SLAB, :]
                    wsu[r:r + SLAB, :] = sgather[cc, xx, yy, zz, SLAB:2 * SLAB, :]
                    wsd[r:r + SLAB, :] = sgather[cc, xx, yy, zz, 2 * SLAB:3 * SLAB, :]
    g = jnp.zeros((COLS, HS), F32)
    u = jnp.zeros((COLS, HS), F32)
    for q in range(NS):
        g = g + dot(x4[q], wsg[q * F:(q + 1) * F, :])
        u = u + dot(x4[q], wsu[q * F:(q + 1) * F, :])
    hs[...] = (silu(g) * u).astype(BF16)

    part_in = []
    for g, (a, b) in enumerate(GROUPS):
        ret_in[g].wait_recv()
        for q in range(a, b):
            part[q] = (dot(wsel[...], ret[q]) + dot_t(hs[...], wsd[q * F:(q + 1) * F, :])).astype(BF16)
        arrivals = []
        for k in LINEK:
            to, frm = line(z, k)
            arrivals.append(remote(part.at[a:b, toks_of(to)], parts.at[a:b, toks_of(z)], parts.at[a:b, toks_of(frm)], psem, (g, k - 1), zdev(to)))
        for q in range(a, b):
            parts[q, toks_of(z), :] = part[q, toks_of(z), :]
        part_in.append(arrivals)

    stores = []
    for g, (a, b) in enumerate(GROUPS):
        for m in part_in[g]:
            m.wait_recv()
        for q in range(a, b):
            total = parts[q, 0:TOK, :].astype(F32)
            for k in range(1, LINE):
                total = total + parts[q, k * TOK:(k + 1) * TOK, :].astype(F32)
            out[:, q * F:(q + 1) * F] = total.astype(BF16)
        stores.append(pltpu.make_async_copy(out.at[:, a * F:b * F], out_hbm.at[:, a * F:b * F], osem.at[g]))
        stores[-1].start()

    for s in sends:
        s.wait_send()
    for s in stores:
        s.wait()


def per_device(tokens, norm_gain, expert_ids, gate_weights, expert_gate, expert_up, expert_down, shared_gate, shared_up, shared_down):
    hbm = pl.BlockSpec(memory_space=pl.ANY)
    dma = pltpu.SemaphoreType.DMA
    return pl.pallas_call(
        kernel,
        out_shape=jax.ShapeDtypeStruct((TOK, D), BF16),
        in_specs=[hbm] * 10,
        out_specs=hbm,
        scratch_shapes=[
            pltpu.VMEM((TOK, D), BF16),
            pltpu.VMEM((1, D), F32),
            pltpu.VMEM((4, TOK), jnp.int32),
            pltpu.VMEM((4, TOK), F32),
            pltpu.VMEM((SLAB, 4 * HS), BF16),
            pltpu.VMEM((SLAB, 4 * HS), BF16),
            pltpu.VMEM((SLAB, 4 * HS), BF16),
            pltpu.VMEM((4, D, DE), BF16),
            pltpu.VMEM((2 * DE, D), BF16),
            pltpu.VMEM((NS, COLS, F), BF16),
            pltpu.VMEM((LINE, 8, TOK), F32),
            pltpu.VMEM((4, 3 * SLAB, HS), BF16),
            pltpu.VMEM((2, 4, 4, 4, 3 * SLAB, HS), BF16),
            pltpu.VMEM((D, HS), BF16),
            pltpu.VMEM((D, HS), BF16),
            pltpu.VMEM((D, HS), BF16),
            pltpu.VMEM((128, COLS), BF16),
            pltpu.VMEM((3, COLS, 128), BF16),
            pltpu.VMEM((ROWS, COLS), BF16),
            pltpu.VMEM((COLS, ROWS), BF16),
            pltpu.VMEM((PEERS, 1, 128), F32),
            pltpu.VMEM((PEERS, 1, 128), F32),
            pltpu.VMEM((NS, ROWS, F), BF16),
            pltpu.VMEM((NS, ROWS, F), BF16),
            pltpu.VMEM((4, ROWS, DE), F32),
            pltpu.VMEM((ROWS, 2 * DE), BF16),
            pltpu.VMEM((NS, ROWS, F), BF16),
            pltpu.VMEM((NS, ROWS, F), BF16),
            pltpu.VMEM((COLS, HS), BF16),
            pltpu.VMEM((NS, COLS, F), BF16),
            pltpu.VMEM((NS, COLS, F), BF16),
            pltpu.VMEM((TOK, D), BF16),
            dma((7,)),
            dma((6,)),
            dma((NG,)),
            dma((2, 3)),
            dma((2, 16)),
            dma((2, NG, 3)),
            dma((2,)),
            dma((2, NG)),
            dma((2, NG)),
            dma((2, NG, 3)),
        ],
        compiler_params=pltpu.CompilerParams(
            collective_id=0, has_side_effects=True, vmem_limit_bytes=67043328
        ),
        name="moe",
    )(
        tokens, norm_gain.reshape(1, D), expert_ids.T, gate_weights.T,
        shared_gate, shared_up, shared_down.T, expert_gate, expert_up, expert_down,
    )


def solution(mesh):
    ep = P("ep")
    return jax.shard_map(
        per_device,
        mesh=mesh,
        in_specs=(ep, P(), ep, ep, ep, ep, ep, ep, ep, P(None, "ep")),
        out_specs=ep,
        check_vma=False,
    )
```

```python
import jax
import jax.numpy as jnp
from jax import lax
from jax.experimental import pallas as pl
from jax.experimental.pallas import tpu as pltpu
from jax.sharding import PartitionSpec as P

EPS = 1e-06
MESH = pl.DeviceIdType.MESH
F32, BF16 = jnp.float32, jnp.bfloat16

D = 2048
DE = 512
SIZES = [256, 512, 512, 512, 256]
NG = len(SIZES)
SETS = [[0, 1], [2, 3], [4]]
SPANS = [slice(sum(SIZES[:g]), sum(SIZES[:g + 1])) for g in range(NG)]
LINE = 4
TOK = 128
CAP = 6
BLK = LINE * CAP
PEERS = 32
ROWS = PEERS * BLK
HALF = ROWS // 2
COLS = LINE * TOK
HS = 128
SLAB = 16

_CHIP = [(0, 1), (1, 0), (0, 3), (3, 0), (1, 1), (1, 3), (3, 1), (3, 3), (0, 2), (2, 0), (2, 1), (1, 2), (2, 3), (3, 2), (2, 2)]
PLANE = [[(a, b, 0) for a, b in _CHIP], [(0, 0, 1)] + [(a, b, 1) for a, b in _CHIP]]
EARLY = 1
HEAD = 3
LINEK = (1, 3, 2)


def silu(v):
    return (0.5 * v) * (1.0 + jnp.tanh(0.5 * v))


def dot(a, b):
    return jnp.dot(a, b, preferred_element_type=F32)


def dot_t(a, b):
    return lax.dot_general(a, b, (((1,), (1,)), ((), ())), preferred_element_type=F32)


def row_pattern(shape, dim, offset):
    row = (lax.broadcasted_iota(jnp.int32, shape, dim) + offset).astype(F32)
    peer = jnp.floor((row + 0.5) * (1.0 / BLK))
    inner = row - BLK * peer
    line = jnp.floor((inner + 0.5) * (1.0 / CAP))
    slot = inner - CAP * line
    return peer, inner, 8.0 * line + slot + 1.0


def kernel(
    tok_hbm, gain_hbm, ids_hbm, gw_hbm, sg_hbm, su_hbm, sd_hbm, wg_hbm, wu_hbm, wd_hbm, out_hbm,
    tok, gain, ids, gw, sg, su, sd,
    wgu, wd, x4, meta, sown, sgather, wsg, wsu, wsd, vmat, bits, sel, wsel, lab_out, lab_in,
    send, got, gu, hid, back, ret, hs, part, parts, out,
    isem, wsem, osem, msem, ssem, xsem, lsem, dsem, rsem, psem,
):
    me = lax.axis_index("ep")
    z, y, x, c = lax.div(me, 32), lax.rem(lax.div(me, 8), 4), lax.rem(lax.div(me, 2), 4), lax.rem(me, 2)
    mine = lax.rem(me, 32)
    sends = []

    def copy_to(src, dst, sems, at, dev):
        return pltpu.make_async_remote_copy(src, dst, sems.at[(0,) + at], sems.at[(1,) + at], device_id=(dev,), device_id_type=MESH)

    def remote(src, dst, landed, sems, at, dev):
        go = copy_to(src, dst, sems, at, dev)
        go.start()
        sends.append(go)
        return copy_to(src, landed, sems, at, dev)

    def line(v, k):
        return lax.rem(v + k, 4), lax.rem(v + 4 - k, 4)

    def zdev(zz):
        return zz * 32 + mine

    def pdev(yy, xx, cc):
        return z * 32 + yy * 8 + xx * 2 + cc

    spot = y * 4 + x
    plane = []
    for h in range(2):
        plane.append([])
        for dy, dx, dc in PLANE[h]:
            chip = lax.rem(y + dy, 4) * 4 + lax.rem(x + dx, 4)
            plane[h].append((h * 16 + chip, z * 32 + chip * 2 + lax.rem(c + dc, 2)))
    everyone = plane[0] + plane[1]

    def rows_of(b):
        return pl.ds(pl.multiple_of(b * BLK, 8), BLK)

    def toks_of(zz):
        return pl.ds(pl.multiple_of(zz * TOK, TOK), TOK)

    def exchange(src, dst, group, h, sems):
        src, dst = src[group], dst[group]
        for to, dev in plane[h]:
            copy_to(src.at[rows_of(to)], dst.at[rows_of(h * 16 + spot)], sems, (group, h), dev).start()
        if h == 0:
            dst[rows_of(spot), :] = src[rows_of(spot), :]
        every = pl.ds(0, len(plane[h]) * BLK)
        done = copy_to(src.at[every], dst.at[every], sems, (group, h), plane[h][0][1])
        sends.append(done)
        return done

    small = [
        pltpu.make_async_copy(src, dst, isem.at[i])
        for i, (src, dst) in enumerate(
            [(tok_hbm, tok), (gain_hbm, gain), (ids_hbm, ids), (gw_hbm, gw), (sg_hbm, sg), (su_hbm, su), (sd_hbm, sd)]
        )
    ]
    for m in small:
        m.start()

    barrier = pltpu.get_barrier_semaphore()
    for k in LINEK:
        pl.semaphore_signal(barrier, inc=1, device_id=(zdev(line(z, k)[0]),), device_id_type=MESH)
    for _, dev in everyone:
        pl.semaphore_signal(barrier, inc=1, device_id=(dev,), device_id_type=MESH)

    weights = []
    for e in range(2):
        weights.append(pltpu.make_async_copy(wg_hbm.at[e], wgu.at[2 * e], wsem.at[3 * e]))
        weights.append(pltpu.make_async_copy(wu_hbm.at[e], wgu.at[2 * e + 1], wsem.at[3 * e + 1]))
    for e in range(2):
        weights.append(pltpu.make_async_copy(wd_hbm.at[e], wd.at[pl.ds(e * DE, DE)], wsem.at[3 * e + 2]))
    for m in small:
        m.wait()
    for w in weights:
        w.start()

    meta[z, 0:4, :] = ids[...].astype(F32)
    meta[z, 4:8, :] = gw[...]
    for q in range(4):
        cut = slice(q * HS, (q + 1) * HS)
        sown[x, y, q, 0:SLAB, :] = sg[:, cut]
        sown[x, y, q, SLAB:2 * SLAB, :] = su[:, cut]
        sown[x, y, q, 2 * SLAB:3 * SLAB, :] = sd[:, cut]

    def norm_tile(i, carry):
        r = pl.ds(pl.multiple_of(i * 16, 16), 16)
        t = tok[r, :].astype(F32)
        t = t * lax.rsqrt(jnp.mean(t * t, axis=-1, keepdims=True) + EPS)
        t = (t * gain[...]).astype(BF16)
        at = pl.ds(pl.multiple_of(z * TOK + i * 16, 16), 16)
        for g in range(NG):
            x4[g][at, :] = t[:, SPANS[g]]
        return carry

    lax.fori_loop(0, TOK // 16, norm_tile, 0)

    pl.semaphore_wait(barrier, len(LINEK) + len(everyone))

    meta_in, slab_1, slab_2, slab_z, x_in = [], [], [], [], [[] for _ in range(NG)]
    half = 3 * SLAB // 2
    top, low = pl.ds(0, half), pl.ds(half, half)
    for k in LINEK:
        to, frm = line(y, k)
        slab_1.append(remote(sown.at[x, y, :, top], sown.at[x, y, :, top], sown.at[x, frm, :, top], ssem, (k - 1,), pdev(to, x, c)))
        to, frm = line(x, k)
        slab_1.append(remote(sown.at[x, y, :, low], sown.at[x, y, :, low], sown.at[frm, y, :, low], ssem, (2 + k,), pdev(y, to, c)))
    for k in LINEK:
        to, frm = line(z, k)
        meta_in.append(remote(meta.at[z], meta.at[z], meta.at[frm], msem, (k - 1,), zdev(to)))
    for g in range(NG):
        for k in LINEK:
            to, frm = line(z, k)
            x_in[g].append(remote(x4[g].at[toks_of(z)], x4[g].at[toks_of(z)], x4[g].at[toks_of(frm)], xsem, (g, k - 1), zdev(to)))

    for m in meta_in:
        m.wait_recv()
    peer = lax.broadcasted_iota(jnp.int32, (PEERS, TOK), 0)
    other = peer >= 16
    here = (z * PEERS + jnp.where(other, peer - 16, peer) * 2 + jnp.where(other, 1 - c, c)).astype(F32)
    before = (
        lax.broadcasted_iota(jnp.int32, (TOK, TOK), 0) < lax.broadcasted_iota(jnp.int32, (TOK, TOK), 1)
    ).astype(F32).astype(BF16)
    wvals, slots, whichs = [], [], []
    for q in range(LINE):
        hit = jnp.zeros((PEERS, TOK), F32)
        wv = jnp.zeros((PEERS, TOK), F32)
        bit = jnp.zeros((PEERS, TOK), F32)
        for k in range(4):
            e = meta[q, k:k + 1, :]
            dev = jnp.floor(e * 0.5)
            is_k = (here == dev).astype(F32)
            hit = hit + is_k
            wv = wv + is_k * meta[q, 4 + k:5 + k, :]
            bit = bit + is_k * (e - 2.0 * dev)
        rank = dot(hit.astype(BF16), before)
        slots.append(jnp.where(hit > 0.0, rank + (8.0 * q + 1.0), 0.0))
        wvals.append(wv)
        whichs.append(bit)

    pad = jnp.zeros((128 - PEERS, TOK), F32)
    for q in range(LINE):
        cut = slice(q * TOK, (q + 1) * TOK)
        vmat[:, cut] = jnp.concatenate([slots[q], pad], axis=0).astype(BF16)

    for m in slab_1:
        m.wait_recv()
    for k in LINEK:
        to, frm = line(x, k)
        slab_2.append(remote(sown.at[x, :, :, top], sown.at[x, :, :, top], sown.at[frm, :, :, top], ssem, (5 + k,), pdev(y, to, c)))
        to, frm = line(y, k)
        slab_2.append(remote(sown.at[:, y, :, low], sown.at[:, y, :, low], sown.at[:, frm, :, low], ssem, (8 + k,), pdev(to, x, c)))

    def sel_tile(i, carry):
        peer, _, target = row_pattern((128, 128), 0, i * 128)
        pick = (peer == lax.broadcasted_iota(jnp.int32, (128, 128), 1).astype(F32)).astype(F32).astype(BF16)
        val = dot(pick, vmat[...])
        sel[pl.ds(pl.multiple_of(i * 128, 128), 128), :] = (val == target[:, 0:1]).astype(F32).astype(BF16)
        return carry

    lax.fori_loop(0, ROWS // 128, sel_tile, 0)

    def dispatch(g):
        for m in x_in[g]:
            m.wait_recv()
        send[g][...] = dot(sel[...], x4[g][...]).astype(BF16)
        return exchange(send, got, g, 0, dsem)

    got_in = [[], []]
    for g in range(EARLY):
        got_in[0].append(dispatch(g))
        got_in[1].append(exchange(send, got, g, 1, dsem))
    got_in[0].append(dispatch(EARLY))

    lane = lax.broadcasted_iota(jnp.int32, (PEERS, 128), 1)
    labels = jnp.zeros((PEERS, 128), F32)
    for q in range(LINE):
        for s in range(CAP):
            bit = jnp.sum(jnp.where(slots[q] == 8.0 * q + s + 1.0, whichs[q], 0.0), axis=1, keepdims=True)
            labels = jnp.where(lane == q * CAP + s, bit, labels)
    for b in range(PEERS):
        lab_out[b] = labels[b:b + 1, :]
    lab_in[spot] = lab_out[spot]
    for h in range(2):
        for to, dev in plane[h]:
            copy_to(lab_out.at[to], lab_in.at[h * 16 + spot], lsem, (), dev).start()
    every = pl.ds(0, len(everyone))
    label_in = copy_to(lab_out.at[every], lab_in.at[every], lsem, (), everyone[0][1])
    sends.append(label_in)
    for q in range(LINE):
        cut = slice(q * TOK, (q + 1) * TOK)
        bits[0, cut, :] = jnp.transpose(jnp.concatenate([slots[q], pad], axis=0)).astype(BF16)
        bits[1, cut, :] = jnp.transpose(jnp.concatenate([wvals[q], pad], axis=0)).astype(BF16)

    for g in range(EARLY + 1, NG):
        got_in[0].append(dispatch(g))
    for g in range(EARLY, NG):
        got_in[1].append(exchange(send, got, g, 1, dsem))
    for m in slab_2:
        m.wait_recv()
    for k in LINEK:
        to, frm = line(z, k)
        slab_z.append(remote(sown.at[:, :, to], sgather.at[c, z], sgather.at[c, frm], ssem, (11 + k,), zdev(to)))
    sgather[c, z] = sown[:, :, z]

    def wsel_tile(i, carry):
        peer, _, target = row_pattern((128, 128), 1, i * 128)
        pick = (peer == lax.broadcasted_iota(jnp.int32, (128, 128), 0).astype(F32)).astype(F32).astype(BF16)
        val = dot(bits[0], pick)
        w = dot(bits[1], pick)
        wsel[:, pl.ds(pl.multiple_of(i * 128, 128), 128)] = jnp.where(val == target[0:1, :], w, 0.0).astype(BF16)
        return carry

    lax.fori_loop(0, ROWS // 128, wsel_tile, 0)

    for w in weights:
        w.wait()
    label_in.wait_recv()
    for b in range(PEERS):
        bits[2, b:b + 1, :] = lab_in[b].astype(BF16)
    peer, inner, _ = row_pattern((ROWS, 128), 0, 0)
    lane = lax.broadcasted_iota(jnp.int32, (ROWS, 128), 1).astype(F32)
    pick = (peer == lane).astype(F32)
    lab = dot(pick.astype(BF16)[:, 0:PEERS], bits[2, 0:PEERS, :])
    which = jnp.sum(jnp.where(inner == lane, lab, 0.0), axis=1, keepdims=True)

    def experts(h):
        rows = slice(h * HALF, (h + 1) * HALF)

        def partial(groups, q, cut):
            return sum(dot(got[g][rows, :], wgu[q, SPANS[g], cut]) for g in groups)

        for n, groups in enumerate(SETS[:-1]):
            for g in groups:
                got_in[h][g].wait_recv()

            def accumulate(q, carry, n=n, groups=groups):
                prod = partial(groups, q, slice(None))
                if n == 0:
                    gu[q, rows, :] = prod
                else:
                    gu[q, rows, :] += prod
                return carry

            lax.fori_loop(0, 4, accumulate, 0)

        for g in SETS[-1]:
            got_in[h][g].wait_recv()
        for e in range(2):
            keep = which[rows] if e == 1 else 1.0 - which[rows]
            for n in range(2):
                cut = slice(n * 256, (n + 1) * 256)
                g = gu[2 * e, rows, cut] + partial(SETS[-1], 2 * e, cut)
                u = gu[2 * e + 1, rows, cut] + partial(SETS[-1], 2 * e + 1, cut)
                hid[rows, e * DE + n * 256:e * DE + (n + 1) * 256] = (silu(g) * u * keep).astype(BF16)

    ret_in = [[] for _ in range(NG)]

    def give_back(g, h):
        rows = slice(h * HALF, (h + 1) * HALF)
        back[g][rows, :] = dot(hid[rows, :], wd[:, SPANS[g]]).astype(BF16)
        ret_in[g].append(exchange(back, ret, g, h, rsem))

    experts(0)
    for g in range(HEAD):
        give_back(g, 0)
    experts(1)
    for g in range(HEAD):
        give_back(g, 1)
    for g in range(HEAD, NG):
        give_back(g, 0)
        give_back(g, 1)

    for m in slab_z:
        m.wait_recv()
    slab_c = remote(sgather.at[c], sgather.at[c], sgather.at[1 - c], ssem, (15,), pdev(y, x, 1 - c))
    slab_c.wait_recv()
    for zz in range(4):
        for yy in range(4):
            for xx in range(4):
                for cc in range(2):
                    r = (((zz * 4 + yy) * 4 + xx) * 2 + cc) * SLAB
                    wsg[r:r + SLAB, :] = sgather[cc, zz, xx, yy, 0:SLAB, :]
                    wsu[r:r + SLAB, :] = sgather[cc, zz, xx, yy, SLAB:2 * SLAB, :]
                    wsd[r:r + SLAB, :] = sgather[cc, zz, xx, yy, 2 * SLAB:3 * SLAB, :]
    g = jnp.zeros((COLS, HS), F32)
    u = jnp.zeros((COLS, HS), F32)
    for q in range(NG):
        g = g + dot(x4[q][...], wsg[SPANS[q], :])
        u = u + dot(x4[q][...], wsu[SPANS[q], :])
    hs[...] = (silu(g) * u).astype(BF16)

    part_in = []
    for g in range(NG):
        for m in ret_in[g]:
            m.wait_recv()
        part[g][...] = (dot(wsel[...], ret[g][...]) + dot_t(hs[...], wsd[SPANS[g], :])).astype(BF16)
        arrivals = []
        for k in LINEK:
            to, frm = line(z, k)
            arrivals.append(remote(part[g].at[toks_of(to)], parts[g].at[toks_of(z)], parts[g].at[toks_of(frm)], psem, (g, k - 1), zdev(to)))
        parts[g][toks_of(z), :] = part[g][toks_of(z), :]
        part_in.append(arrivals)

    stores = []
    for g in range(NG):
        for m in part_in[g]:
            m.wait_recv()
        total = parts[g][0:TOK, :].astype(F32)
        for k in range(1, LINE):
            total = total + parts[g][k * TOK:(k + 1) * TOK, :].astype(F32)
        out[:, SPANS[g]] = total.astype(BF16)
        stores.append(pltpu.make_async_copy(out.at[:, SPANS[g]], out_hbm.at[:, SPANS[g]], osem.at[g]))
        stores[-1].start()

    for s in sends:
        s.wait_send()
    for s in stores:
        s.wait()


def per_device(tokens, norm_gain, expert_ids, gate_weights, expert_gate, expert_up, expert_down, shared_gate, shared_up, shared_down):
    hbm = pl.BlockSpec(memory_space=pl.ANY)
    dma = pltpu.SemaphoreType.DMA

    def per_group(rows):
        return [pltpu.VMEM((rows, f), BF16) for f in SIZES]

    return pl.pallas_call(
        kernel,
        out_shape=jax.ShapeDtypeStruct((TOK, D), BF16),
        in_specs=[hbm] * 10,
        out_specs=hbm,
        scratch_shapes=[
            pltpu.VMEM((TOK, D), BF16),
            pltpu.VMEM((1, D), F32),
            pltpu.VMEM((4, TOK), jnp.int32),
            pltpu.VMEM((4, TOK), F32),
            pltpu.VMEM((SLAB, 4 * HS), BF16),
            pltpu.VMEM((SLAB, 4 * HS), BF16),
            pltpu.VMEM((SLAB, 4 * HS), BF16),
            pltpu.VMEM((4, D, DE), BF16),
            pltpu.VMEM((2 * DE, D), BF16),
            per_group(COLS),
            pltpu.VMEM((LINE, 8, TOK), F32),
            pltpu.VMEM((4, 4, 4, 3 * SLAB, HS), BF16),
            pltpu.VMEM((2, 4, 4, 4, 3 * SLAB, HS), BF16),
            pltpu.VMEM((D, HS), BF16),
            pltpu.VMEM((D, HS), BF16),
            pltpu.VMEM((D, HS), BF16),
            pltpu.VMEM((128, COLS), BF16),
            pltpu.VMEM((3, COLS, 128), BF16),
            pltpu.VMEM((ROWS, COLS), BF16),
            pltpu.VMEM((COLS, ROWS), BF16),
            pltpu.VMEM((PEERS, 1, 128), F32),
            pltpu.VMEM((PEERS, 1, 128), F32),
            per_group(ROWS),
            per_group(ROWS),
            pltpu.VMEM((4, ROWS, DE), F32),
            pltpu.VMEM((ROWS, 2 * DE), BF16),
            per_group(ROWS),
            per_group(ROWS),
            pltpu.VMEM((COLS, HS), BF16),
            per_group(COLS),
            per_group(COLS),
            pltpu.VMEM((TOK, D), BF16),
            dma((7,)),
            dma((6,)),
            dma((NG,)),
            dma((2, 3)),
            dma((2, 16)),
            dma((2, NG, 3)),
            dma((2,)),
            dma((2, NG, 2)),
            dma((2, NG, 2)),
            dma((2, NG, 3)),
        ],
        compiler_params=pltpu.CompilerParams(
            collective_id=0, has_side_effects=True, vmem_limit_bytes=67043328
        ),
        name="moe",
    )(
        tokens, norm_gain.reshape(1, D), expert_ids.T, gate_weights.T,
        shared_gate, shared_up, shared_down.T, expert_gate, expert_up, expert_down,
    )


def solution(mesh):
    ep = P("ep")
    return jax.shard_map(
        per_device,
        mesh=mesh,
        in_specs=(ep, P(), ep, ep, ep, ep, ep, ep, ep, P(None, "ep")),
        out_specs=ep,
        check_vma=False,
    )
```

```python
import jax
import jax.numpy as jnp
from jax import lax
from jax.experimental import pallas as pl
from jax.experimental.pallas import tpu as pltpu
from jax.sharding import PartitionSpec as P

EPS = 1e-06
MESH = pl.DeviceIdType.MESH
F32, BF16 = jnp.float32, jnp.bfloat16

D = 2048
DE = 512
SIZES = [256, 512, 512, 384, 384]
NG = len(SIZES)
SETS = [[0, 1], [2, 3], [4]]
SPANS = [slice(sum(SIZES[:g]), sum(SIZES[:g + 1])) for g in range(NG)]
LINE = 4
TOK = 128
CAP = 6
BLK = LINE * CAP
PEERS = 32
ROWS = PEERS * BLK
HALF = ROWS // 2
COLS = LINE * TOK
HS = 128
SLAB = 16

_CHIP = [(0, 1), (1, 0), (0, 3), (3, 0), (1, 1), (1, 3), (3, 1), (3, 3), (0, 2), (2, 0), (2, 1), (1, 2), (2, 3), (3, 2), (2, 2)]
PLANE = [[(a, b, 0) for a, b in _CHIP], [(0, 0, 1)] + [(a, b, 1) for a, b in _CHIP]]
EARLY = 1
HEAD = 3
LINEK = (1, 3, 2)


def silu(v):
    return (0.5 * v) * (1.0 + jnp.tanh(0.5 * v))


def dot(a, b):
    return jnp.dot(a, b, preferred_element_type=F32)


def dot_t(a, b):
    return lax.dot_general(a, b, (((1,), (1,)), ((), ())), preferred_element_type=F32)


def row_pattern(shape, dim, offset):
    row = (lax.broadcasted_iota(jnp.int32, shape, dim) + offset).astype(F32)
    peer = jnp.floor((row + 0.5) * (1.0 / BLK))
    inner = row - BLK * peer
    line = jnp.floor((inner + 0.5) * (1.0 / CAP))
    slot = inner - CAP * line
    return peer, inner, 8.0 * line + slot + 1.0


def kernel(
    tok_hbm, gain_hbm, ids_hbm, gw_hbm, sg_hbm, su_hbm, sd_hbm, wg_hbm, wu_hbm, wd_hbm, out_hbm,
    tok, gain, ids, gw, sg, su, sd,
    wgu, wd, x4, meta, sown, sgather, wsg, wsu, wsd, vmat, bits, sel, wsel, lab_out, lab_in,
    send, got, gu, hid, back, ret, hs, part, parts, out,
    isem, wsem, osem, msem, ssem, xsem, lsem, dsem, rsem, psem,
):
    me = lax.axis_index("ep")
    z, y, x, c = lax.div(me, 32), lax.rem(lax.div(me, 8), 4), lax.rem(lax.div(me, 2), 4), lax.rem(me, 2)
    mine = lax.rem(me, 32)
    sends = []

    def copy_to(src, dst, sems, at, dev):
        return pltpu.make_async_remote_copy(src, dst, sems.at[(0,) + at], sems.at[(1,) + at], device_id=(dev,), device_id_type=MESH)

    def remote(src, dst, landed, sems, at, dev):
        go = copy_to(src, dst, sems, at, dev)
        go.start()
        sends.append(go)
        return copy_to(src, landed, sems, at, dev)

    def line(v, k):
        return lax.rem(v + k, 4), lax.rem(v + 4 - k, 4)

    def zdev(zz):
        return zz * 32 + mine

    def pdev(yy, xx, cc):
        return z * 32 + yy * 8 + xx * 2 + cc

    spot = y * 4 + x
    plane = []
    for h in range(2):
        plane.append([])
        for dy, dx, dc in PLANE[h]:
            chip = lax.rem(y + dy, 4) * 4 + lax.rem(x + dx, 4)
            plane[h].append((h * 16 + chip, z * 32 + chip * 2 + lax.rem(c + dc, 2)))
    everyone = plane[0] + plane[1]

    def rows_of(b):
        return pl.ds(pl.multiple_of(b * BLK, 8), BLK)

    def toks_of(zz):
        return pl.ds(pl.multiple_of(zz * TOK, TOK), TOK)

    def exchange(src, dst, group, h, sems):
        src, dst = src[group], dst[group]
        for to, dev in plane[h]:
            copy_to(src.at[rows_of(to)], dst.at[rows_of(h * 16 + spot)], sems, (group, h), dev).start()
        if h == 0:
            dst[rows_of(spot), :] = src[rows_of(spot), :]
        every = pl.ds(0, len(plane[h]) * BLK)
        done = copy_to(src.at[every], dst.at[every], sems, (group, h), plane[h][0][1])
        sends.append(done)
        return done

    small = [
        pltpu.make_async_copy(src, dst, isem.at[i])
        for i, (src, dst) in enumerate(
            [(tok_hbm, tok), (gain_hbm, gain), (ids_hbm, ids), (gw_hbm, gw), (sg_hbm, sg), (su_hbm, su), (sd_hbm, sd)]
        )
    ]
    for m in small:
        m.start()

    barrier = pltpu.get_barrier_semaphore()
    for k in LINEK:
        pl.semaphore_signal(barrier, inc=1, device_id=(zdev(line(z, k)[0]),), device_id_type=MESH)
    for _, dev in everyone:
        pl.semaphore_signal(barrier, inc=1, device_id=(dev,), device_id_type=MESH)

    weights = []
    for e in range(2):
        weights.append(pltpu.make_async_copy(wg_hbm.at[e], wgu.at[2 * e], wsem.at[3 * e]))
        weights.append(pltpu.make_async_copy(wu_hbm.at[e], wgu.at[2 * e + 1], wsem.at[3 * e + 1]))
    for e in range(2):
        weights.append(pltpu.make_async_copy(wd_hbm.at[e], wd.at[pl.ds(e * DE, DE)], wsem.at[3 * e + 2]))
    for m in small:
        m.wait()
    for w in weights:
        w.start()

    meta[z, 0:4, :] = ids[...].astype(F32)
    meta[z, 4:8, :] = gw[...]
    for q in range(4):
        cut = slice(q * HS, (q + 1) * HS)
        sown[x, y, q, 0:SLAB, :] = sg[:, cut]
        sown[x, y, q, SLAB:2 * SLAB, :] = su[:, cut]
        sown[x, y, q, 2 * SLAB:3 * SLAB, :] = sd[:, cut]

    def norm_tile(i, carry):
        r = pl.ds(pl.multiple_of(i * 16, 16), 16)
        t = tok[r, :].astype(F32)
        t = t * lax.rsqrt(jnp.mean(t * t, axis=-1, keepdims=True) + EPS)
        t = (t * gain[...]).astype(BF16)
        at = pl.ds(pl.multiple_of(z * TOK + i * 16, 16), 16)
        for g in range(NG):
            x4[g][at, :] = t[:, SPANS[g]]
        return carry

    lax.fori_loop(0, TOK // 16, norm_tile, 0)

    pl.semaphore_wait(barrier, len(LINEK) + len(everyone))

    meta_in, slab_1, slab_2, slab_z, x_in = [], [], [], [], [[] for _ in range(NG)]
    half = 3 * SLAB // 2
    top, low = pl.ds(0, half), pl.ds(half, half)
    for k in LINEK:
        to, frm = line(y, k)
        slab_1.append(remote(sown.at[x, y, :, top], sown.at[x, y, :, top], sown.at[x, frm, :, top], ssem, (k - 1,), pdev(to, x, c)))
        to, frm = line(x, k)
        slab_1.append(remote(sown.at[x, y, :, low], sown.at[x, y, :, low], sown.at[frm, y, :, low], ssem, (2 + k,), pdev(y, to, c)))
    for k in LINEK:
        to, frm = line(z, k)
        meta_in.append(remote(meta.at[z], meta.at[z], meta.at[frm], msem, (k - 1,), zdev(to)))
    for g in range(NG):
        for k in LINEK:
            to, frm = line(z, k)
            x_in[g].append(remote(x4[g].at[toks_of(z)], x4[g].at[toks_of(z)], x4[g].at[toks_of(frm)], xsem, (g, k - 1), zdev(to)))

    for m in meta_in:
        m.wait_recv()
    peer = lax.broadcasted_iota(jnp.int32, (PEERS, TOK), 0)
    other = peer >= 16
    here = (z * PEERS + jnp.where(other, peer - 16, peer) * 2 + jnp.where(other, 1 - c, c)).astype(F32)
    before = (
        lax.broadcasted_iota(jnp.int32, (TOK, TOK), 0) < lax.broadcasted_iota(jnp.int32, (TOK, TOK), 1)
    ).astype(F32).astype(BF16)
    wvals, slots, whichs = [], [], []
    for q in range(LINE):
        hit = jnp.zeros((PEERS, TOK), F32)
        wv = jnp.zeros((PEERS, TOK), F32)
        bit = jnp.zeros((PEERS, TOK), F32)
        for k in range(4):
            e = meta[q, k:k + 1, :]
            dev = jnp.floor(e * 0.5)
            is_k = (here == dev).astype(F32)
            hit = hit + is_k
            wv = wv + is_k * meta[q, 4 + k:5 + k, :]
            bit = bit + is_k * (e - 2.0 * dev)
        rank = dot(hit.astype(BF16), before)
        slots.append(jnp.where(hit > 0.0, rank + (8.0 * q + 1.0), 0.0))
        wvals.append(wv)
        whichs.append(bit)

    pad = jnp.zeros((128 - PEERS, TOK), F32)
    for q in range(LINE):
        cut = slice(q * TOK, (q + 1) * TOK)
        vmat[:, cut] = jnp.concatenate([slots[q], pad], axis=0).astype(BF16)

    for m in slab_1:
        m.wait_recv()
    for k in LINEK:
        to, frm = line(x, k)
        slab_2.append(remote(sown.at[x, :, :, top], sown.at[x, :, :, top], sown.at[frm, :, :, top], ssem, (5 + k,), pdev(y, to, c)))
        to, frm = line(y, k)
        slab_2.append(remote(sown.at[:, y, :, low], sown.at[:, y, :, low], sown.at[:, frm, :, low], ssem, (8 + k,), pdev(to, x, c)))

    def sel_tile(i, carry):
        peer, _, target = row_pattern((128, 128), 0, i * 128)
        pick = (peer == lax.broadcasted_iota(jnp.int32, (128, 128), 1).astype(F32)).astype(F32).astype(BF16)
        val = dot(pick, vmat[...])
        sel[pl.ds(pl.multiple_of(i * 128, 128), 128), :] = (val == target[:, 0:1]).astype(F32).astype(BF16)
        return carry

    lax.fori_loop(0, ROWS // 128, sel_tile, 0)

    def dispatch(g):
        for m in x_in[g]:
            m.wait_recv()
        send[g][...] = dot(sel[...], x4[g][...]).astype(BF16)
        return exchange(send, got, g, 0, dsem)

    got_in = [[], []]
    for g in range(EARLY):
        got_in[0].append(dispatch(g))
        got_in[1].append(exchange(send, got, g, 1, dsem))
    got_in[0].append(dispatch(EARLY))

    lane = lax.broadcasted_iota(jnp.int32, (PEERS, 128), 1)
    labels = jnp.zeros((PEERS, 128), F32)
    for q in range(LINE):
        for s in range(CAP):
            bit = jnp.sum(jnp.where(slots[q] == 8.0 * q + s + 1.0, whichs[q], 0.0), axis=1, keepdims=True)
            labels = jnp.where(lane == q * CAP + s, bit, labels)
    for b in range(PEERS):
        lab_out[b] = labels[b:b + 1, :]
    lab_in[spot] = lab_out[spot]
    for h in range(2):
        for to, dev in plane[h]:
            copy_to(lab_out.at[to], lab_in.at[h * 16 + spot], lsem, (), dev).start()
    every = pl.ds(0, len(everyone))
    label_in = copy_to(lab_out.at[every], lab_in.at[every], lsem, (), everyone[0][1])
    sends.append(label_in)
    for q in range(LINE):
        cut = slice(q * TOK, (q + 1) * TOK)
        bits[0, cut, :] = jnp.transpose(jnp.concatenate([slots[q], pad], axis=0)).astype(BF16)
        bits[1, cut, :] = jnp.transpose(jnp.concatenate([wvals[q], pad], axis=0)).astype(BF16)

    for g in range(EARLY + 1, NG):
        got_in[0].append(dispatch(g))
    for g in range(EARLY, NG):
        got_in[1].append(exchange(send, got, g, 1, dsem))
    for m in slab_2:
        m.wait_recv()
    for k in LINEK:
        to, frm = line(z, k)
        slab_z.append(remote(sown.at[:, :, to], sgather.at[c, z], sgather.at[c, frm], ssem, (11 + k,), zdev(to)))
    sgather[c, z] = sown[:, :, z]

    def wsel_tile(i, carry):
        peer, _, target = row_pattern((128, 128), 1, i * 128)
        pick = (peer == lax.broadcasted_iota(jnp.int32, (128, 128), 0).astype(F32)).astype(F32).astype(BF16)
        val = dot(bits[0], pick)
        w = dot(bits[1], pick)
        wsel[:, pl.ds(pl.multiple_of(i * 128, 128), 128)] = jnp.where(val == target[0:1, :], w, 0.0).astype(BF16)
        return carry

    lax.fori_loop(0, ROWS // 128, wsel_tile, 0)

    for w in weights:
        w.wait()
    label_in.wait_recv()
    for b in range(PEERS):
        bits[2, b:b + 1, :] = lab_in[b].astype(BF16)
    peer, inner, _ = row_pattern((ROWS, 128), 0, 0)
    lane = lax.broadcasted_iota(jnp.int32, (ROWS, 128), 1).astype(F32)
    pick = (peer == lane).astype(F32)
    lab = dot(pick.astype(BF16)[:, 0:PEERS], bits[2, 0:PEERS, :])
    which = jnp.sum(jnp.where(inner == lane, lab, 0.0), axis=1, keepdims=True)

    def experts(h):
        rows = slice(h * HALF, (h + 1) * HALF)

        def partial(groups, q, cut):
            return sum(dot(got[g][rows, :], wgu[q, SPANS[g], cut]) for g in groups)

        for n, groups in enumerate(SETS[:-1]):
            for g in groups:
                got_in[h][g].wait_recv()

            def accumulate(q, carry, n=n, groups=groups):
                prod = partial(groups, q, slice(None))
                if n == 0:
                    gu[q, rows, :] = prod
                else:
                    gu[q, rows, :] += prod
                return carry

            lax.fori_loop(0, 4, accumulate, 0)

        for g in SETS[-1]:
            got_in[h][g].wait_recv()
        for e in range(2):
            keep = which[rows] if e == 1 else 1.0 - which[rows]
            for n in range(2):
                cut = slice(n * 256, (n + 1) * 256)
                g = gu[2 * e, rows, cut] + partial(SETS[-1], 2 * e, cut)
                u = gu[2 * e + 1, rows, cut] + partial(SETS[-1], 2 * e + 1, cut)
                hid[rows, e * DE + n * 256:e * DE + (n + 1) * 256] = (silu(g) * u * keep).astype(BF16)

    ret_in = [[] for _ in range(NG)]

    def give_back(g, h):
        rows = slice(h * HALF, (h + 1) * HALF)
        back[g][rows, :] = dot(hid[rows, :], wd[:, SPANS[g]]).astype(BF16)
        ret_in[g].append(exchange(back, ret, g, h, rsem))

    experts(0)
    for g in range(HEAD):
        give_back(g, 0)
    experts(1)
    for g in range(HEAD):
        give_back(g, 1)
    for g in range(HEAD, NG):
        give_back(g, 0)
        give_back(g, 1)

    for m in slab_z:
        m.wait_recv()
    slab_c = remote(sgather.at[c], sgather.at[c], sgather.at[1 - c], ssem, (15,), pdev(y, x, 1 - c))
    slab_c.wait_recv()
    for zz in range(4):
        for yy in range(4):
            for xx in range(4):
                for cc in range(2):
                    r = (((zz * 4 + yy) * 4 + xx) * 2 + cc) * SLAB
                    wsg[r:r + SLAB, :] = sgather[cc, zz, xx, yy, 0:SLAB, :]
                    wsu[r:r + SLAB, :] = sgather[cc, zz, xx, yy, SLAB:2 * SLAB, :]
                    wsd[r:r + SLAB, :] = sgather[cc, zz, xx, yy, 2 * SLAB:3 * SLAB, :]
    g = jnp.zeros((COLS, HS), F32)
    u = jnp.zeros((COLS, HS), F32)
    for q in range(NG):
        g = g + dot(x4[q][...], wsg[SPANS[q], :])
        u = u + dot(x4[q][...], wsu[SPANS[q], :])
    hs[...] = (silu(g) * u).astype(BF16)

    part_in = []
    for g in range(NG):
        for m in ret_in[g]:
            m.wait_recv()
        part[g][...] = (dot(wsel[...], ret[g][...]) + dot_t(hs[...], wsd[SPANS[g], :])).astype(BF16)
        arrivals = []
        for k in LINEK:
            to, frm = line(z, k)
            arrivals.append(remote(part[g].at[toks_of(to)], parts[g].at[toks_of(z)], parts[g].at[toks_of(frm)], psem, (g, k - 1), zdev(to)))
        parts[g][toks_of(z), :] = part[g][toks_of(z), :]
        part_in.append(arrivals)

    stores = []
    for g in range(NG):
        for m in part_in[g]:
            m.wait_recv()
        total = parts[g][0:TOK, :].astype(F32)
        for k in range(1, LINE):
            total = total + parts[g][k * TOK:(k + 1) * TOK, :].astype(F32)
        out[:, SPANS[g]] = total.astype(BF16)
        stores.append(pltpu.make_async_copy(out.at[:, SPANS[g]], out_hbm.at[:, SPANS[g]], osem.at[g]))
        stores[-1].start()

    for s in sends:
        s.wait_send()
    for s in stores:
        s.wait()


def per_device(tokens, norm_gain, expert_ids, gate_weights, expert_gate, expert_up, expert_down, shared_gate, shared_up, shared_down):
    hbm = pl.BlockSpec(memory_space=pl.ANY)
    dma = pltpu.SemaphoreType.DMA

    def per_group(rows):
        return [pltpu.VMEM((rows, f), BF16) for f in SIZES]

    return pl.pallas_call(
        kernel,
        out_shape=jax.ShapeDtypeStruct((TOK, D), BF16),
        in_specs=[hbm] * 10,
        out_specs=hbm,
        scratch_shapes=[
            pltpu.VMEM((TOK, D), BF16),
            pltpu.VMEM((1, D), F32),
            pltpu.VMEM((4, TOK), jnp.int32),
            pltpu.VMEM((4, TOK), F32),
            pltpu.VMEM((SLAB, 4 * HS), BF16),
            pltpu.VMEM((SLAB, 4 * HS), BF16),
            pltpu.VMEM((SLAB, 4 * HS), BF16),
            pltpu.VMEM((4, D, DE), BF16),
            pltpu.VMEM((2 * DE, D), BF16),
            per_group(COLS),
            pltpu.VMEM((LINE, 8, TOK), F32),
            pltpu.VMEM((4, 4, 4, 3 * SLAB, HS), BF16),
            pltpu.VMEM((2, 4, 4, 4, 3 * SLAB, HS), BF16),
            pltpu.VMEM((D, HS), BF16),
            pltpu.VMEM((D, HS), BF16),
            pltpu.VMEM((D, HS), BF16),
            pltpu.VMEM((128, COLS), BF16),
            pltpu.VMEM((3, COLS, 128), BF16),
            pltpu.VMEM((ROWS, COLS), BF16),
            pltpu.VMEM((COLS, ROWS), BF16),
            pltpu.VMEM((PEERS, 1, 128), F32),
            pltpu.VMEM((PEERS, 1, 128), F32),
            per_group(ROWS),
            per_group(ROWS),
            pltpu.VMEM((4, ROWS, DE), F32),
            pltpu.VMEM((ROWS, 2 * DE), BF16),
            per_group(ROWS),
            per_group(ROWS),
            pltpu.VMEM((COLS, HS), BF16),
            per_group(COLS),
            per_group(COLS),
            pltpu.VMEM((TOK, D), BF16),
            dma((7,)),
            dma((6,)),
            dma((NG,)),
            dma((2, 3)),
            dma((2, 16)),
            dma((2, NG, 3)),
            dma((2,)),
            dma((2, NG, 2)),
            dma((2, NG, 2)),
            dma((2, NG, 3)),
        ],
        compiler_params=pltpu.CompilerParams(
            collective_id=0, has_side_effects=True, vmem_limit_bytes=67043328
        ),
        name="moe",
    )(
        tokens, norm_gain.reshape(1, D), expert_ids.T, gate_weights.T,
        shared_gate, shared_up, shared_down.T, expert_gate, expert_up, expert_down,
    )


def solution(mesh):
    ep = P("ep")
    return jax.shard_map(
        per_device,
        mesh=mesh,
        in_specs=(ep, P(), ep, ep, ep, ep, ep, ep, ep, P(None, "ep")),
        out_specs=ep,
        check_vma=False,
    )
```
